32 devices in a mesh: ep: 8 (over z, y), tp: 4 (over x, core).
Axes of the slice: x: 2, y: 2, z: 4, core: 2. Of those that a mesh axis runs over, the one named last changes fastest.
Arguments:
- tokens: bfloat16 [1024, 2048], P('ep'), may hold values from -6 to 6
- norm_gain: float32 [2048], replicated, may hold values from 0.1 to 1.9
- routes: int32 [1024, 2], P('ep'), may hold values from 0 to 7, as said below
- route_scores: float32 [1024, 2], P('ep'), may hold values from -6 to 6
- expert_gate: bfloat16 [8, 2048, 4096], P('ep', None, 'tp'), may hold values from -0.125 to 0.125
- expert_up: bfloat16 [8, 2048, 4096], P('ep', None, 'tp'), may hold values from -0.125 to 0.125
- expert_down: bfloat16 [8, 4096, 2048], P('ep', None, 'tp'), may hold values from -0.09375 to 0.09375
- branch_in: bfloat16 [2048, 512], P('ep', 'tp'), may hold values from -0.125 to 0.125
- branch_out: bfloat16 [512, 2048], P('tp', 'ep'), may hold values from -0.25 to 0.25
- branch_gate: float32 [2048], replicated, may hold values from -0.125 to 0.125
Outputs:
- mixed: bfloat16 [1024, 2048], P('ep', 'tp')
The draws below stay inside these ranges and needn't reach their ends.
Inputs may be any that keep to these rules, and one draw needn't show every extreme that they name: `routes`: each row names 2 different experts. In each aligned block of 128 rows (the rows of one index of ep) no expert is named more than 40 times, and one expert, the same in every block, is named exactly 40 times in every block.
All inputs are finite; a program needn't handle non-finite values.
Results may differ from the reference program's by a relative error of at most 0.0066.
Values may be sent and summed in bfloat16 or wider, within the bound.
No kernel may reach another device: no remote copies, remote signals or barrier semaphores. Data moves between devices by JAX's collectives and lax.ppermute only.
A program may use at most 64 MiB of HBM per device.

```python
from functools import partial
import jax
import jax.numpy as jnp
from jax import lax

D = 2048
FF = 4096
DB = 512
TOP = 2
TOK_DEV = 128
GROUP = 1
EXPERTS = 8
FF_PART = 4096
CAP = 40
TOKENS = 1024
N_EP = 8


def route_block(block_key, popular, full_expert):
    pool_size = EXPERTS * CAP
    pool = jnp.arange(pool_size, dtype=jnp.int32) // CAP
    noise_key, order_key = jax.random.split(block_key)
    noise = jax.random.randint(noise_key, (pool_size,), 0, 64, dtype=jnp.int32)
    serial = jnp.arange(pool_size, dtype=jnp.int32)
    score = (noise + popular[pool]) * pool_size + serial
    score = jnp.where(pool == full_expert, 200 * pool_size + serial, score)
    ranked = jnp.argsort(-score, stable=True)
    kept = jnp.sort(ranked[:TOP * TOK_DEV])
    chosen = pool[kept]
    pairs = jnp.stack([chosen[:TOK_DEV], chosen[TOK_DEV:]], axis=1)
    shuffle = jax.random.permutation(order_key, TOK_DEV)
    return pairs[shuffle]


def draw_routes(key, part):
    base = jax.random.fold_in(key, 7)
    full_key, popular_key, block_key = jax.random.split(base, 3)
    full_expert = jax.random.randint(full_key, (), 0, EXPERTS, dtype=jnp.int32)
    popular = jax.random.randint(popular_key, (EXPERTS,), 0, 48, dtype=jnp.int32)
    block_keys = jax.random.split(block_key, TOKENS // TOK_DEV)
    blocks = jax.vmap(partial(route_block, popular=popular, full_expert=full_expert))(block_keys)
    return blocks.reshape(TOKENS, TOP).astype(jnp.int32)


def steps_of(rng, shape, pieces, low, largest):
    def one(dim, blocks):
        draws = jax.random.uniform(jax.random.fold_in(jax.random.fold_in(rng, 6), dim), (blocks,), jnp.float32, low / len(pieces), largest / len(pieces))
        return jnp.repeat(jnp.exp(draws), shape[dim] // blocks).reshape((-1,) + (1,) * (len(shape) - dim - 1))

    level = one(*pieces[0])
    for cut in pieces[1:]:
        level = level * one(*cut)
    return level


def scatter_about(key, extent, spread, reach, shards=(), kind=jnp.bfloat16):
    entries = spread * jax.random.normal(key, extent, jnp.float32)
    if shards:
        entries = entries * steps_of(key, extent, shards, -0.22, 0.18)
    return jnp.clip(entries, -reach, reach).astype(kind)


def setup_inputs(seed: int = 0) -> dict:
    streams_of = jax.random.split(jax.random.key(seed), 11)
    tokens = scatter_about(streams_of[0], (TOKENS, D), 1.0, 6.0, ((0, 8),))
    norm_gain = jnp.clip(1.0 + 0.18 * jax.random.normal(streams_of[1], (D,), jnp.float32), 0.1, 1.9)
    routes = draw_routes(jax.random.fold_in(streams_of[10], 71), 0)
    route_scores = scatter_about(streams_of[3], (TOKENS, TOP), 1.5, 6.0, ((0, 8),), jnp.float32)
    expert_gate = scatter_about(streams_of[4], (EXPERTS * GROUP, D, FF_PART), D ** -0.5, 0.125, ((0, 8), (2, 4)))
    expert_up = scatter_about(streams_of[5], (EXPERTS * GROUP, D, FF_PART), D ** -0.5, 0.125, ((0, 8), (2, 4)))
    expert_down = scatter_about(streams_of[6], (EXPERTS * GROUP, FF_PART, D), FF ** -0.5, 0.09375, ((0, 8), (2, 4)))
    branch_in = scatter_about(streams_of[7], (D, DB), D ** -0.5, 0.125, ((0, 8), (1, 4)))
    branch_out = scatter_about(streams_of[8], (DB, D), DB ** -0.5, 0.25, ((0, 4), (1, 8)))
    branch_gate = scatter_about(streams_of[9], (D,), D ** -0.5, 0.125, (), jnp.float32)
    return dict(tokens=tokens, norm_gain=norm_gain, routes=routes, route_scores=route_scores, expert_gate=expert_gate, expert_up=expert_up, expert_down=expert_down, branch_in=branch_in, branch_out=branch_out, branch_gate=branch_gate)


NORM_EPSILON = 1e-06

def reference(tokens, norm_gain, routes, route_scores, expert_gate, expert_up, expert_down, branch_in, branch_out, branch_gate):
    tokens_float = tokens.astype(jnp.float32)
    scaled = lax.rsqrt(lax.optimization_barrier(jnp.mean(tokens_float * tokens_float, axis=-1, keepdims=True)) + NORM_EPSILON)
    normed = (tokens_float * scaled * norm_gain).astype(jnp.bfloat16)
    difference = route_scores[:, 0] - route_scores[:, 1]
    route_weight = jnp.stack([jax.nn.sigmoid(difference), jax.nn.sigmoid(-difference)], axis=1)
    flat_weight = route_weight.reshape(-1)
    blocks = routes.reshape(N_EP, TOK_DEV * TOP)
    choose = (blocks[:, :, None] == jnp.arange(EXPERTS, dtype=jnp.int32)[None, None, :]).astype(jnp.int32)
    earlier = jnp.cumsum(choose, axis=1, dtype=jnp.int32) - choose
    slot_index = lax.optimization_barrier(jnp.sum(earlier * choose, axis=2, dtype=jnp.int32))
    source_base = jnp.arange(N_EP, dtype=jnp.int32)[:, None] * CAP
    slot_place = (source_base + slot_index).reshape(-1).astype(jnp.int32)
    flat_ids = routes.reshape(-1).astype(jnp.int32)
    owner_token = jnp.arange(TOKENS * TOP, dtype=jnp.int32) // TOP

    def one_expert(running, expert):
        selected = flat_ids == expert
        target = jnp.where(selected, slot_place, N_EP * CAP).astype(jnp.int32)
        row_index = jnp.zeros((N_EP * CAP,), jnp.int32).at[target].set(owner_token, mode='drop')
        row_scale = jnp.zeros((N_EP * CAP,), jnp.float32).at[target].set(flat_weight, mode='drop')
        picked = normed[row_index]
        start = (expert * GROUP).astype(jnp.int32)
        gate_block = lax.dynamic_slice_in_dim(expert_gate, start, GROUP, 0)
        gate_block = jnp.transpose(gate_block, (1, 0, 2)).reshape(D, FF)
        up_block = lax.dynamic_slice_in_dim(expert_up, start, GROUP, 0)
        up_block = jnp.transpose(up_block, (1, 0, 2)).reshape(D, FF)
        down_block = lax.dynamic_slice_in_dim(expert_down, start, GROUP, 0).reshape(FF, D)
        gate_pre = jnp.dot(picked, gate_block, preferred_element_type=jnp.float32)
        up_pre = jnp.dot(picked, up_block, preferred_element_type=jnp.float32)
        hidden = (jax.nn.silu(gate_pre) * up_pre).astype(jnp.bfloat16)
        result = jnp.dot(hidden, down_block, preferred_element_type=jnp.float32)
        running = running.at[row_index].add(row_scale[:, None] * result)
        return (running, None)
    routed, _ = lax.scan(one_expert, jnp.zeros((TOKENS, D), jnp.float32), jnp.arange(EXPERTS, dtype=jnp.int32))
    branch_hidden = jax.nn.silu(jnp.dot(normed, branch_in, preferred_element_type=jnp.float32)).astype(jnp.bfloat16)
    branch_value = jnp.dot(branch_hidden, branch_out, preferred_element_type=jnp.float32)
    branch_weight = jax.nn.sigmoid(lax.optimization_barrier(jnp.sum(normed.astype(jnp.float32) * branch_gate, axis=-1)))
    return (routed + branch_weight[:, None] * branch_value).astype(jnp.bfloat16)
```

```python
import jax
import jax.numpy as jnp
from jax import lax
from jax.experimental import pallas as pl
from jax.experimental.pallas import tpu as pltpu
from jax.sharding import PartitionSpec as P

NORM_EPSILON = 1e-06
BF = jnp.bfloat16
F32 = jnp.float32
VMEM_BYTES = 40 * 1024 * 1024


def send(x, axis, offset):
    if offset == 0:
        return x
    count = lax.axis_size(axis)
    return lax.ppermute(x, axis, [(i, i ^ offset) for i in range(count)])


def relay(x):
    core = send(x, "tp", 1)
    far = send(x, "tp", 2)
    return [x, core, far, send(far, "tp", 1)]


def call(body, out_shape, scratch, cost, *args):
    scalar = pl.BlockSpec(memory_space=pltpu.SMEM)
    vector = pl.BlockSpec(memory_space=pltpu.VMEM)
    multi = isinstance(out_shape, (list, tuple))
    return pl.pallas_call(
        body,
        out_shape=out_shape,
        in_specs=[scalar] + [vector] * (len(args) - 1),
        out_specs=[vector] * len(out_shape) if multi else vector,
        scratch_shapes=scratch,
        compiler_params=pltpu.CompilerParams(vmem_limit_bytes=VMEM_BYTES),
        cost_estimate=pl.CostEstimate(flops=cost, transcendentals=0, bytes_accessed=0),
    )(*args)


def collect(place, blocks, whole, width):
    for offset, block in enumerate(blocks):
        start = pl.multiple_of((place ^ offset) * width, width)
        whole[:, pl.ds(start, width)] = block[...]


def gate_up_body(place_ref, b0, b1, b2, b3, gate_ref, up_ref, out_ref, whole):
    collect(place_ref[0], (b0, b1, b2, b3), whole, b0.shape[1])
    width = out_ref.shape[1]
    step = min(256, width)
    for start in range(0, width, step):
        cols = pl.ds(start, step)
        gate = jnp.dot(whole[...], gate_ref[0, :, cols], preferred_element_type=F32)
        up = jnp.dot(whole[...], up_ref[0, :, cols], preferred_element_type=F32)
        out_ref[:, cols] = (gate / (1.0 + jnp.exp(-gate)) * up).astype(BF)


def down_body(place_ref, b0, b1, b2, b3, down_ref, out_ref, whole):
    collect(place_ref[0], (b0, b1, b2, b3), whole, b0.shape[1])
    width = out_ref.shape[1]
    step = min(256, width)
    for start in range(0, width, step):
        cols = pl.ds(start, step)
        out_ref[:, cols] = jnp.dot(
            whole[...], down_ref[0, :, cols], preferred_element_type=F32
        ).astype(BF)


def branch_body(place_ref, normed_ref, in_ref, out_ref, terms_ref):
    tp_place, ep_place = place_ref[0], place_ref[1]
    count, depth, _ = in_ref.shape
    width = out_ref.shape[2]
    per_share = terms_ref.shape[2] // width
    total = jnp.zeros((normed_ref.shape[0], in_ref.shape[2]), F32)
    for offset in range(count):
        start = pl.multiple_of((ep_place ^ offset) * depth, depth)
        total += jnp.dot(
            normed_ref[:, pl.ds(start, depth)], in_ref[offset], preferred_element_type=F32
        )
    hidden = (total / (1.0 + jnp.exp(-total))).astype(BF)
    for offset in range(count):
        block = ep_place ^ offset
        share = (block // per_share) ^ tp_place
        start = pl.multiple_of((block % per_share) * width, width)
        terms_ref[share, :, pl.ds(start, width)] = jnp.dot(
            hidden, out_ref[offset], preferred_element_type=F32
        ).astype(BF)


def normalise(tokens, norm_gain):
    tokens_float = tokens.astype(F32)
    scaled = lax.rsqrt(jnp.mean(tokens_float * tokens_float, axis=-1, keepdims=True) + NORM_EPSILON)
    return (tokens_float * scaled * norm_gain).astype(BF)


def slots(routes, route_scores, count, capacity, flip):
    rows = routes.shape[0]
    relative = (routes ^ flip).T
    match = relative[:, None, :] == jnp.arange(count, dtype=jnp.int32)[None, :, None]
    chosen = match[0] | match[1]
    before = (jnp.arange(rows)[:, None] < jnp.arange(rows)[None, :]).astype(BF)
    rank = jnp.dot(chosen.astype(BF), before, preferred_element_type=F32)
    rank = jnp.where(chosen, rank.astype(jnp.int32), -1)
    held = rank[:, None, :] == jnp.arange(capacity, dtype=jnp.int32)[None, :, None]
    difference = route_scores[:, 0] - route_scores[:, 1]
    weight = jnp.where(
        match[0], jax.nn.sigmoid(difference)[None, :], jax.nn.sigmoid(-difference)[None, :]
    )
    spread = jnp.where(held, weight[:, None, :], 0.0).reshape(count * capacity, rows)
    return held.astype(BF).reshape(count * capacity, rows), spread


def combine(spread, per_slot):
    return lax.dot_general(
        spread,
        per_slot.astype(F32),
        (((0,), (0,)), ((), ())),
        precision=lax.Precision.HIGHEST,
        preferred_element_type=F32,
    )


def on_device(
    tokens,
    norm_gain,
    routes,
    route_scores,
    expert_gate,
    expert_up,
    expert_down,
    branch_in,
    branch_out,
    branch_gate,
):
    ep_count = lax.axis_size("ep")
    tp_count = lax.axis_size("tp")
    tok_rows, model_width = tokens.shape
    fanout = routes.shape[1]
    group_size = max(1, ep_count // 32)
    expert_count = ep_count // group_size
    capacity = 5 * tok_rows * fanout // (4 * expert_count)
    column_width = model_width // tp_count
    tp_place = lax.axis_index("tp")
    ep_place = lax.axis_index("ep")
    direct = ep_count <= 8 and tp_count == 4 and group_size == 1

    normed = normalise(tokens, norm_gain)
    own_columns = lax.dynamic_slice_in_dim(normed, tp_place * column_width, column_width, 1)
    held, spread = slots(
        routes, route_scores, expert_count, capacity, ep_place if direct else jnp.int32(0)
    )
    packed = jnp.dot(held, own_columns, preferred_element_type=F32).astype(BF)
    packed = packed.reshape(expert_count, capacity, column_width)
    branch_weight = jax.nn.sigmoid(jnp.sum(normed.astype(F32) * branch_gate, axis=-1))

    if not direct:
        outgoing = jnp.broadcast_to(
            packed[:, None], (expert_count, group_size, capacity, column_width)
        ).reshape(ep_count, capacity, column_width)
        arrived = lax.all_to_all(outgoing, "ep", split_axis=0, concat_axis=0, tiled=True)
        rows = lax.all_gather(arrived.reshape(-1, column_width), "tp", axis=1, tiled=True)
        gate_pre = jnp.dot(rows, expert_gate[0], preferred_element_type=F32)
        up_pre = jnp.dot(rows, expert_up[0], preferred_element_type=F32)
        hidden = (jax.nn.silu(gate_pre) * up_pre).astype(BF)
        hidden = lax.all_gather(hidden, "tp", axis=1, tiled=True)
        partial_out = jnp.dot(hidden, expert_down[0], preferred_element_type=F32)
        partial_out = partial_out.reshape(ep_count, capacity, -1)
        returned = lax.all_to_all(partial_out, "ep", split_axis=0, concat_axis=0, tiled=True)
        per_slot = jnp.sum(returned.reshape(expert_count, group_size, capacity, -1), axis=1)
        routed = combine(spread, per_slot.reshape(expert_count * capacity, -1))
        whole_in = lax.all_gather(branch_in, "ep", axis=0, tiled=True)
        branch_hidden = jax.nn.silu(
            jnp.dot(normed, whole_in, preferred_element_type=F32)
        ).astype(BF)
        whole_out = lax.all_gather(branch_out, "ep", axis=1, tiled=True)
        terms = jnp.dot(branch_hidden, whole_out, preferred_element_type=F32)
        share = lax.psum_scatter(terms, "tp", scatter_dimension=1, tiled=True)
        return (routed + branch_weight[:, None] * share).astype(BF)

    place = jnp.stack([tp_place, ep_place]).astype(jnp.int32)
    half = max(1, ep_count // 2)
    groups = [range(0, half), range(half, ep_count)]
    hidden_width = expert_gate.shape[2]
    out_width = expert_down.shape[2]

    arrivals = []
    for group in groups:
        arrivals.append(jnp.concatenate([send(packed[j], "ep", j) for j in group], axis=0))

    gate_in, gate_out, arrivals[1] = lax.optimization_barrier((branch_in, branch_out, arrivals[1]))
    in_blocks, out_blocks = gate_in[None], gate_out[None]
    for step in (1, 2, 4):
        if step < ep_count:
            in_blocks = jnp.concatenate([in_blocks, send(in_blocks, "ep", step)], axis=0)
            out_blocks = jnp.concatenate([out_blocks, send(out_blocks, "ep", step)], axis=0)

    returned = []
    for group, arrived in zip(groups, arrivals):
        rows = len(group) * capacity
        hidden = call(
            gate_up_body,
            jax.ShapeDtypeStruct((rows, hidden_width), BF),
            [pltpu.VMEM((rows, model_width), BF)],
            4 * rows * model_width * hidden_width,
            place,
            *relay(arrived),
            expert_gate,
            expert_up,
        )
        result = call(
            down_body,
            jax.ShapeDtypeStruct((rows, out_width), BF),
            [pltpu.VMEM((rows, hidden_width * tp_count), BF)],
            2 * rows * hidden_width * tp_count * out_width,
            place,
            *relay(hidden),
            expert_down,
        )
        for slot, j in enumerate(group):
            returned.append(send(result[slot * capacity : (slot + 1) * capacity], "ep", j))

    terms = call(
        branch_body,
        jax.ShapeDtypeStruct((tp_count, tok_rows, out_width), BF),
        [],
        2 * tok_rows * branch_in.shape[1] * 2 * model_width,
        place,
        normed,
        in_blocks,
        out_blocks,
    )
    near = send(jnp.stack([terms[1], terms[3]]), "tp", 1).astype(F32)
    share = terms[0].astype(F32) + near[0]
    other = (terms[2].astype(F32) + near[1]).astype(BF)
    share = share + send(other, "tp", 2).astype(F32)

    routed = combine(spread, jnp.concatenate(returned, axis=0))
    return (routed + branch_weight[:, None] * share).astype(BF)


def solution(mesh):
    in_specs = (
        P("ep", None),
        P(),
        P("ep", None),
        P("ep", None),
        P("ep", None, "tp"),
        P("ep", None, "tp"),
        P("ep", None, "tp"),
        P("ep", "tp"),
        P("tp", "ep"),
        P(),
    )
    out_specs = P("ep", "tp")
    return jax.shard_map(
        on_device, mesh=mesh, in_specs=in_specs, out_specs=out_specs, check_vma=False
    )
```

```python
from functools import partial

import jax
import jax.numpy as jnp
from jax import lax
from jax.experimental import pallas as pl
from jax.experimental.pallas import tpu as pltpu
from jax.sharding import PartitionSpec as P

NORM_EPSILON = 1e-06
BF = jnp.bfloat16
F32 = jnp.float32
VMEM_BYTES = 20 * 1024 * 1024


def send(x, axis, offset):
    if offset == 0:
        return x
    count = lax.axis_size(axis)
    return lax.ppermute(x, axis, [(i, i ^ offset) for i in range(count)])


def relay(x):
    core = send(x, "tp", 1)
    far = send(x, "tp", 2)
    return [x, core, far, send(far, "tp", 1)]


def call(body, out_shape, scratch, cost, *args):
    scalar = pl.BlockSpec(memory_space=pltpu.SMEM)
    vector = pl.BlockSpec(memory_space=pltpu.VMEM)
    multi = isinstance(out_shape, (list, tuple))
    return pl.pallas_call(
        body,
        out_shape=out_shape,
        in_specs=[scalar] + [vector] * (len(args) - 1),
        out_specs=[vector] * len(out_shape) if multi else vector,
        scratch_shapes=scratch,
        compiler_params=pltpu.CompilerParams(vmem_limit_bytes=VMEM_BYTES),
        cost_estimate=pl.CostEstimate(flops=cost, transcendentals=0, bytes_accessed=0),
    )(*args)


def collect(place, blocks, whole, width):
    for offset, block in enumerate(blocks):
        start = pl.multiple_of((place ^ offset) * width, width)
        whole[:, pl.ds(start, width)] = block[...]


def gate_up_body(place_ref, b0, b1, b2, b3, gate_ref, up_ref, out_ref, whole):
    collect(place_ref[0], (b0, b1, b2, b3), whole, b0.shape[1])
    width = out_ref.shape[1]
    step = min(256, width)
    for start in range(0, width, step):
        cols = pl.ds(start, step)
        gate = jnp.dot(whole[...], gate_ref[0, :, cols], preferred_element_type=F32)
        up = jnp.dot(whole[...], up_ref[0, :, cols], preferred_element_type=F32)
        out_ref[:, cols] = (gate / (1.0 + jnp.exp(-gate)) * up).astype(BF)


def down_body(place_ref, b0, b1, b2, b3, down_ref, out_ref, whole):
    collect(place_ref[0], (b0, b1, b2, b3), whole, b0.shape[1])
    width = out_ref.shape[1]
    step = min(256, width)
    for start in range(0, width, step):
        cols = pl.ds(start, step)
        out_ref[:, cols] = jnp.dot(
            whole[...], down_ref[0, :, cols], preferred_element_type=F32
        ).astype(BF)


def branch_body(place_ref, normed_ref, own_ref, lower_ref, upper_ref, far_ref, terms_ref, *, depth):
    tp_place, ep_place, ep_count = place_ref[0], place_ref[1], place_ref[2]
    width = own_ref.shape[2]
    pieces = own_ref.shape[1] // width - depth // width
    per_share = terms_ref.shape[2] // (pieces * width)
    sources = ((own_ref, 0), (lower_ref, -2), (upper_ref, 2), (far_ref, -4))
    blocks = []
    for ref, move in sources:
        base = lax.rem(ep_place + move + ep_count, ep_count)
        blocks += [(ref, 0, base), (ref, 1, base ^ 1)]
    total = jnp.zeros((normed_ref.shape[0], width), F32)
    for ref, side, block in blocks:
        start = pl.multiple_of(block * depth, depth)
        total += jnp.dot(
            normed_ref[:, pl.ds(start, depth)], ref[side, :depth], preferred_element_type=F32
        )
    hidden = (total / (1.0 + jnp.exp(-total))).astype(BF)
    for ref, side, block in blocks:
        share = (block // per_share) ^ tp_place
        for piece in range(pieces):
            start = pl.multiple_of(((block % per_share) * pieces + piece) * width, width)
            rows = pl.ds(depth + piece * width, width)
            terms_ref[share, :, pl.ds(start, width)] = jnp.dot(
                hidden, ref[side, rows], preferred_element_type=F32
            ).astype(BF)


def normalise(tokens, norm_gain):
    tokens_float = tokens.astype(F32)
    scaled = lax.rsqrt(jnp.mean(tokens_float * tokens_float, axis=-1, keepdims=True) + NORM_EPSILON)
    return (tokens_float * scaled * norm_gain).astype(BF)


def slots(routes, route_scores, count, capacity, flip):
    rows = routes.shape[0]
    relative = (routes ^ flip).T
    match = relative[:, None, :] == jnp.arange(count, dtype=jnp.int32)[None, :, None]
    chosen = match[0] | match[1]
    before = (jnp.arange(rows)[:, None] < jnp.arange(rows)[None, :]).astype(BF)
    rank = jnp.dot(chosen.astype(BF), before, preferred_element_type=F32)
    rank = jnp.where(chosen, rank.astype(jnp.int32), -1)
    held = rank[:, None, :] == jnp.arange(capacity, dtype=jnp.int32)[None, :, None]
    difference = route_scores[:, 0] - route_scores[:, 1]
    weight = jnp.where(
        match[0], jax.nn.sigmoid(difference)[None, :], jax.nn.sigmoid(-difference)[None, :]
    )
    spread = jnp.where(held, weight[:, None, :], 0.0).reshape(count * capacity, rows)
    return held.astype(BF).reshape(count * capacity, rows), spread


def combine(spread, per_slot):
    return lax.dot_general(
        spread,
        per_slot.astype(F32),
        (((0,), (0,)), ((), ())),
        precision=lax.Precision.HIGHEST,
        preferred_element_type=F32,
    )


def on_device(
    tokens,
    norm_gain,
    routes,
    route_scores,
    expert_gate,
    expert_up,
    expert_down,
    branch_in,
    branch_out,
    branch_gate,
):
    ep_count = lax.axis_size("ep")
    tp_count = lax.axis_size("tp")
    tok_rows, model_width = tokens.shape
    fanout = routes.shape[1]
    group_size = max(1, ep_count // 32)
    expert_count = ep_count // group_size
    capacity = 5 * tok_rows * fanout // (4 * expert_count)
    column_width = model_width // tp_count
    tp_place = lax.axis_index("tp")
    ep_place = lax.axis_index("ep")
    direct = ep_count == 8 and tp_count == 4

    if direct:
        width = branch_in.shape[1]
        cuts = [branch_out[:, k : k + width] for k in range(0, branch_out.shape[1], width)]
        weights = jnp.concatenate([branch_in] + cuts, axis=0)
        pair = jnp.stack([weights, send(weights, "ep", 1)])
    normed = normalise(tokens, norm_gain)
    own_columns = lax.dynamic_slice_in_dim(normed, tp_place * column_width, column_width, 1)
    held, spread = slots(
        routes, route_scores, expert_count, capacity, ep_place if direct else jnp.int32(0)
    )
    packed = jnp.dot(held, own_columns, preferred_element_type=F32).astype(BF)
    packed = packed.reshape(expert_count, capacity, column_width)
    branch_weight = jax.nn.sigmoid(jnp.sum(normed.astype(F32) * branch_gate, axis=-1))

    if not direct:
        outgoing = jnp.broadcast_to(
            packed[:, None], (expert_count, group_size, capacity, column_width)
        ).reshape(ep_count, capacity, column_width)
        arrived = lax.all_to_all(outgoing, "ep", split_axis=0, concat_axis=0, tiled=True)
        rows = lax.all_gather(arrived.reshape(-1, column_width), "tp", axis=1, tiled=True)
        gate_pre = jnp.dot(rows, expert_gate[0], preferred_element_type=F32)
        up_pre = jnp.dot(rows, expert_up[0], preferred_element_type=F32)
        hidden = (jax.nn.silu(gate_pre) * up_pre).astype(BF)
        hidden = lax.all_gather(hidden, "tp", axis=1, tiled=True)
        partial_out = jnp.dot(hidden, expert_down[0], preferred_element_type=F32)
        partial_out = partial_out.reshape(ep_count, capacity, -1)
        returned = lax.all_to_all(partial_out, "ep", split_axis=0, concat_axis=0, tiled=True)
        per_slot = jnp.sum(returned.reshape(expert_count, group_size, capacity, -1), axis=1)
        routed = combine(spread, per_slot.reshape(expert_count * capacity, -1))
        whole_in = lax.all_gather(branch_in, "ep", axis=0, tiled=True)
        branch_hidden = jax.nn.silu(
            jnp.dot(normed, whole_in, preferred_element_type=F32)
        ).astype(BF)
        whole_out = lax.all_gather(branch_out, "ep", axis=1, tiled=True)
        terms = jnp.dot(branch_hidden, whole_out, preferred_element_type=F32)
        share = lax.psum_scatter(terms, "tp", scatter_dimension=1, tiled=True)
        return (routed + branch_weight[:, None] * share).astype(BF)

    place = jnp.stack([tp_place, ep_place, ep_count]).astype(jnp.int32)
    half = ep_count // 2
    groups = [range(half, ep_count), range(0, half)]
    hidden_width = expert_gate.shape[2]
    out_width = expert_down.shape[2]

    def shift(x, move):
        return lax.ppermute(x, "ep", [(i, (i + move) % ep_count) for i in range(ep_count)])

    arrivals = []
    for group in groups:
        arrivals.append(jnp.concatenate([send(packed[j], "ep", j) for j in group], axis=0))

    gathered, returned = None, []
    for group, arrived in zip(groups, arrivals):
        rows = len(group) * capacity
        hidden = call(
            gate_up_body,
            jax.ShapeDtypeStruct((rows, hidden_width), BF),
            [pltpu.VMEM((rows, model_width), BF)],
            4 * rows * model_width * hidden_width,
            place,
            *relay(arrived),
            expert_gate,
            expert_up,
        )
        if gathered is None:
            pair, hidden = lax.optimization_barrier((pair, hidden))
            lower, upper = shift(pair, 2), shift(pair, -2)
            gathered = [pair, lower, upper, shift(lower, 2)]
        result = call(
            down_body,
            jax.ShapeDtypeStruct((rows, out_width), BF),
            [pltpu.VMEM((rows, hidden_width * tp_count), BF)],
            2 * rows * hidden_width * tp_count * out_width,
            place,
            *relay(hidden),
            expert_down,
        )
        if not returned:
            normed, result = lax.optimization_barrier((normed, result))
            terms = call(
                partial(branch_body, depth=branch_in.shape[0]),
                jax.ShapeDtypeStruct((tp_count, tok_rows, out_width), BF),
                [],
                2 * tok_rows * branch_in.shape[1] * 2 * model_width,
                place,
                normed,
                *gathered,
            )
        for slot, j in enumerate(group):
            block = result[slot * capacity : (slot + 1) * capacity]
            returned.append((j, send(block, "ep", j)))

    near = send(jnp.stack([terms[1], terms[3]]), "tp", 1).astype(F32)
    share = terms[0].astype(F32) + near[0]
    other = (terms[2].astype(F32) + near[1]).astype(BF)
    share = share + send(other, "tp", 2).astype(F32)

    routed = combine(
        spread, jnp.concatenate([block for _, block in sorted(returned, key=lambda r: r[0])], axis=0)
    )
    return (routed + branch_weight[:, None] * share).astype(BF)


def solution(mesh):
    in_specs = (
        P("ep", None),
        P(),
        P("ep", None),
        P("ep", None),
        P("ep", None, "tp"),
        P("ep", None, "tp"),
        P("ep", None, "tp"),
        P("ep", "tp"),
        P("tp", "ep"),
        P(),
    )
    out_specs = P("ep", "tp")
    return jax.shard_map(
        on_device, mesh=mesh, in_specs=in_specs, out_specs=out_specs, check_vma=False
    )
```

```python
from functools import partial

import jax
import jax.numpy as jnp
from jax import lax
from jax.experimental import pallas as pl
from jax.experimental.pallas import tpu as pltpu
from jax.sharding import PartitionSpec as P

NORM_EPSILON = 1e-06
BF = jnp.bfloat16
F32 = jnp.float32
VMEM_BYTES = 20 * 1024 * 1024
PACK_COST = 1 << 34


def send(x, axis, offset):
    if offset == 0:
        return x
    count = lax.axis_size(axis)
    return lax.ppermute(x, axis, [(i, i ^ offset) for i in range(count)])


def relay(x, after=None):
    far = send(x, "tp", 2)
    core = send(x, "tp", 1)
    if after is not None:
        far, core, after = lax.optimization_barrier((far, core, after))
    return [x, core, far, send(far, "tp", 1)], after


def pack_body(place_ref, held_ref, columns_ref, packed_ref):
    packed_ref[...] = jnp.dot(
        held_ref[...], columns_ref[...], preferred_element_type=F32
    ).astype(BF)


def call(body, out_shape, scratch, cost, *args):
    scalar = pl.BlockSpec(memory_space=pltpu.SMEM)
    vector = pl.BlockSpec(memory_space=pltpu.VMEM)
    multi = isinstance(out_shape, (list, tuple))
    return pl.pallas_call(
        body,
        out_shape=out_shape,
        in_specs=[scalar] + [vector] * (len(args) - 1),
        out_specs=[vector] * len(out_shape) if multi else vector,
        scratch_shapes=scratch,
        compiler_params=pltpu.CompilerParams(vmem_limit_bytes=VMEM_BYTES),
        cost_estimate=pl.CostEstimate(flops=cost, transcendentals=0, bytes_accessed=0),
    )(*args)


def collect(place, blocks, whole, width):
    for offset, block in enumerate(blocks):
        start = pl.multiple_of((place ^ offset) * width, width)
        whole[:, pl.ds(start, width)] = block[...]


def gate_up_body(place_ref, b0, b1, b2, b3, gate_ref, up_ref, out_ref, whole):
    collect(place_ref[0], (b0, b1, b2, b3), whole, b0.shape[1])
    width = out_ref.shape[1]
    step = min(256, width)
    for start in range(0, width, step):
        cols = pl.ds(start, step)
        gate = jnp.dot(whole[...], gate_ref[0, :, cols], preferred_element_type=F32)
        up = jnp.dot(whole[...], up_ref[0, :, cols], preferred_element_type=F32)
        out_ref[:, cols] = (gate / (1.0 + jnp.exp(-gate)) * up).astype(BF)


def down_body(place_ref, b0, b1, b2, b3, down_ref, out_ref, whole):
    collect(place_ref[0], (b0, b1, b2, b3), whole, b0.shape[1])
    width = out_ref.shape[1]
    step = min(256, width)
    for start in range(0, width, step):
        cols = pl.ds(start, step)
        out_ref[:, cols] = jnp.dot(
            whole[...], down_ref[0, :, cols], preferred_element_type=F32
        ).astype(BF)


def branch_body(place_ref, normed_ref, own_ref, lower_ref, upper_ref, far_ref, terms_ref, *, depth):
    tp_place, ep_place, ep_count = place_ref[0], place_ref[1], place_ref[2]
    width = own_ref.shape[2]
    pieces = own_ref.shape[1] // width - depth // width
    per_share = terms_ref.shape[2] // (pieces * width)
    sources = ((own_ref, 0), (lower_ref, -2), (upper_ref, 2), (far_ref, 4))
    blocks = []
    for ref, move in sources:
        base = lax.rem(ep_place + move + ep_count, ep_count)
        blocks += [(ref, 0, base), (ref, 1, base ^ 1)]
    total = jnp.zeros((normed_ref.shape[0], width), F32)
    for ref, side, block in blocks:
        start = pl.multiple_of(block * depth, depth)
        total += jnp.dot(
            normed_ref[:, pl.ds(start, depth)], ref[side, :depth], preferred_element_type=F32
        )
    hidden = (total / (1.0 + jnp.exp(-total))).astype(BF)
    for ref, side, block in blocks:
        share = (block // per_share) ^ tp_place
        for piece in range(pieces):
            start = pl.multiple_of(((block % per_share) * pieces + piece) * width, width)
            rows = pl.ds(depth + piece * width, width)
            terms_ref[share, :, pl.ds(start, width)] = jnp.dot(
                hidden, ref[side, rows], preferred_element_type=F32
            ).astype(BF)


def normalise(tokens, norm_gain):
    tokens_float = tokens.astype(F32)
    scaled = lax.rsqrt(jnp.mean(tokens_float * tokens_float, axis=-1, keepdims=True) + NORM_EPSILON)
    return (tokens_float * scaled * norm_gain).astype(BF)


def slots(routes, route_scores, count, capacity, flip):
    rows = routes.shape[0]
    relative = (routes ^ flip).T
    match = relative[:, None, :] == jnp.arange(count, dtype=jnp.int32)[None, :, None]
    chosen = match[0] | match[1]
    before = (jnp.arange(rows)[:, None] < jnp.arange(rows)[None, :]).astype(BF)
    rank = jnp.dot(chosen.astype(BF), before, preferred_element_type=F32)
    rank = jnp.where(chosen, rank.astype(jnp.int32), -1)
    held = rank[:, None, :] == jnp.arange(capacity, dtype=jnp.int32)[None, :, None]
    difference = route_scores[:, 0] - route_scores[:, 1]
    weight = jnp.where(
        match[0], jax.nn.sigmoid(difference)[None, :], jax.nn.sigmoid(-difference)[None, :]
    )
    spread = jnp.where(held, weight[:, None, :], 0.0).reshape(count * capacity, rows)
    return held.astype(BF).reshape(count * capacity, rows), spread


def combine(spread, per_slot):
    return lax.dot_general(
        spread,
        per_slot.astype(F32),
        (((0,), (0,)), ((), ())),
        precision=lax.Precision.HIGHEST,
        preferred_element_type=F32,
    )


def on_device(
    tokens,
    norm_gain,
    routes,
    route_scores,
    expert_gate,
    expert_up,
    expert_down,
    branch_in,
    branch_out,
    branch_gate,
):
    ep_count = lax.axis_size("ep")
    tp_count = lax.axis_size("tp")
    tok_rows, model_width = tokens.shape
    fanout = routes.shape[1]
    group_size = max(1, ep_count // 32)
    expert_count = ep_count // group_size
    capacity = 5 * tok_rows * fanout // (4 * expert_count)
    column_width = model_width // tp_count
    tp_place = lax.axis_index("tp")
    ep_place = lax.axis_index("ep")
    direct = ep_count == 8 and tp_count == 4

    if direct:
        width = branch_in.shape[1]
        cuts = [branch_out[:, k : k + width] for k in range(0, branch_out.shape[1], width)]
        weights = jnp.concatenate([branch_in] + cuts, axis=0)
        pair = jnp.stack([weights, send(weights, "ep", 1)])
    normed = normalise(tokens, norm_gain)
    own_columns = lax.dynamic_slice_in_dim(normed, tp_place * column_width, column_width, 1)
    held, spread = slots(
        routes, route_scores, expert_count, capacity, ep_place if direct else jnp.int32(0)
    )
    if direct:
        pair, held = lax.optimization_barrier((pair, held))
        place = jnp.stack([tp_place, ep_place, ep_count]).astype(jnp.int32)
        packed = call(
            pack_body,
            jax.ShapeDtypeStruct((held.shape[0], column_width), BF),
            [],
            PACK_COST,
            place,
            held,
            own_columns,
        )
    else:
        packed = jnp.dot(held, own_columns, preferred_element_type=F32).astype(BF)
    packed = packed.reshape(expert_count, capacity, column_width)
    branch_weight = jax.nn.sigmoid(jnp.sum(normed.astype(F32) * branch_gate, axis=-1))

    if not direct:
        outgoing = jnp.broadcast_to(
            packed[:, None], (expert_count, group_size, capacity, column_width)
        ).reshape(ep_count, capacity, column_width)
        arrived = lax.all_to_all(outgoing, "ep", split_axis=0, concat_axis=0, tiled=True)
        rows = lax.all_gather(arrived.reshape(-1, column_width), "tp", axis=1, tiled=True)
        gate_pre = jnp.dot(rows, expert_gate[0], preferred_element_type=F32)
        up_pre = jnp.dot(rows, expert_up[0], preferred_element_type=F32)
        hidden = (jax.nn.silu(gate_pre) * up_pre).astype(BF)
        hidden = lax.all_gather(hidden, "tp", axis=1, tiled=True)
        partial_out = jnp.dot(hidden, expert_down[0], preferred_element_type=F32)
        partial_out = partial_out.reshape(ep_count, capacity, -1)
        returned = lax.all_to_all(partial_out, "ep", split_axis=0, concat_axis=0, tiled=True)
        per_slot = jnp.sum(returned.reshape(expert_count, group_size, capacity, -1), axis=1)
        routed = combine(spread, per_slot.reshape(expert_count * capacity, -1))
        whole_in = lax.all_gather(branch_in, "ep", axis=0, tiled=True)
        branch_hidden = jax.nn.silu(
            jnp.dot(normed, whole_in, preferred_element_type=F32)
        ).astype(BF)
        whole_out = lax.all_gather(branch_out, "ep", axis=1, tiled=True)
        terms = jnp.dot(branch_hidden, whole_out, preferred_element_type=F32)
        share = lax.psum_scatter(terms, "tp", scatter_dimension=1, tiled=True)
        return (routed + branch_weight[:, None] * share).astype(BF)

    half = ep_count // 2
    groups = [range(0, half), range(half, ep_count)]
    hidden_width = expert_gate.shape[2]
    out_width = expert_down.shape[2]

    def shift(x, move):
        return lax.ppermute(x, "ep", [(i, (i + move) % ep_count) for i in range(ep_count)])

    arrivals = []
    for group in groups:
        arrivals.append(jnp.concatenate([send(packed[j], "ep", j) for j in group], axis=0))

    pair, arrivals[1] = lax.optimization_barrier((pair, arrivals[1]))
    gathered = [pair] + [shift(pair, move) for move in (2, -2, 4)]

    returned, result = [], None
    for group, arrived in zip(groups, arrivals):
        rows = len(group) * capacity
        hidden = call(
            gate_up_body,
            jax.ShapeDtypeStruct((rows, hidden_width), BF),
            [pltpu.VMEM((rows, model_width), BF)],
            4 * rows * model_width * hidden_width,
            place,
            *relay(arrived)[0],
            expert_gate,
            expert_up,
        )
        pieces, result = relay(hidden, result)
        result = call(
            down_body,
            jax.ShapeDtypeStruct((rows, out_width), BF),
            [pltpu.VMEM((rows, hidden_width * tp_count), BF)],
            2 * rows * hidden_width * tp_count * out_width,
            place,
            *pieces,
            expert_down,
        )
        for slot, j in enumerate(group):
            block = result[slot * capacity : (slot + 1) * capacity]
            returned.append((j, send(block, "ep", j)))
        if group is groups[0]:
            normed, result = lax.optimization_barrier((normed, result))
            terms = call(
                partial(branch_body, depth=branch_in.shape[0]),
                jax.ShapeDtypeStruct((tp_count, tok_rows, out_width), BF),
                [],
                2 * tok_rows * branch_in.shape[1] * 2 * model_width,
                place,
                normed,
                *gathered,
            )

    near = send(jnp.stack([terms[1], terms[3]]), "tp", 1).astype(F32)
    share = terms[0].astype(F32) + near[0]
    other = (terms[2].astype(F32) + near[1]).astype(BF)
    share = share + send(other, "tp", 2).astype(F32)

    routed = combine(
        spread, jnp.concatenate([block for _, block in sorted(returned, key=lambda r: r[0])], axis=0)
    )
    return (routed + branch_weight[:, None] * share).astype(BF)


def solution(mesh):
    in_specs = (
        P("ep", None),
        P(),
        P("ep", None),
        P("ep", None),
        P("ep", None, "tp"),
        P("ep", None, "tp"),
        P("ep", None, "tp"),
        P("ep", "tp"),
        P("tp", "ep"),
        P(),
    )
    out_specs = P("ep", "tp")
    return jax.shard_map(
        on_device, mesh=mesh, in_specs=in_specs, out_specs=out_specs, check_vma=False
    )
```
